32 devices in a mesh: sp: 8 (over z, y), tp: 4 (over x, core).
Axes of the slice: x: 2, y: 2, z: 4, core: 2. Of those that a mesh axis runs over, the one named last changes fastest.
Arguments:
- stream: bfloat16 [1024, 2048], P('sp', 'tp'), may hold values from -40 to 40
- queries: bfloat16 [1024, 1024], P('sp', 'tp'), may hold values from -6 to 6
- keys: bfloat16 [1024, 1024], P('sp', 'tp'), may hold values from -6 to 6
- values: bfloat16 [1024, 2048], P('sp', 'tp'), may hold values from -25 to 25
- out_gate: bfloat16 [1024, 2048], P('sp', 'tp'), may hold values from -8 to 8
- input_gate: float32 [1024, 8], P('sp', 'tp'), may hold values from -9 to 350
- forget_gate: float32 [1024, 8], P('sp', 'tp'), may hold values from -4 to 20
- head_gain: float32 [2048], P('tp'), may hold values from 0.1 to 1.9
- w_out: bfloat16 [2048, 2048], P('tp'), may hold values from -0.125 to 0.125
- ffn_gain: float32 [2048], replicated, may hold values from 0.1 to 1.9
- w_gate: bfloat16 [2048, 5632], P('sp', 'tp'), may hold values from -0.125 to 0.125
- w_up: bfloat16 [2048, 5632], P('sp', 'tp'), may hold values from -0.125 to 0.125
- w_down: bfloat16 [5632, 2048], P('tp', 'sp'), may hold values from -0.078125 to 0.078125
Outputs:
- mixed: bfloat16 [1024, 2048], P('sp', 'tp')
The draws below stay inside these ranges and needn't reach their ends.
All inputs are finite; a program needn't handle non-finite values.
Results may differ from the reference program's by a relative error of at most 0.0095.
Values may be sent and summed in bfloat16 or wider, within the bound.
No kernel may reach another device: no remote copies, remote signals or barrier semaphores. Data moves between devices by JAX's collectives and lax.ppermute only.
A program may use at most 128 MiB of HBM per device.

```python
import math
import jax
import jax.numpy as jnp
from jax import lax

D = 2048
HEADS = 8
DQK = 128
DV = 256
FF = 5632
BLOCK = 64
TOK_DEV = 128
SEQUENCE_TOKENS = 1024
VALS = 2048
N_SP = 8
N_TP = 4


def draw_stream(key, part):
    first, second = jax.random.split(jax.random.fold_in(key, 11), 2)
    rising = 3.0 ** (jnp.arange(D, dtype=jnp.float32) / D)
    rough = jnp.exp(jax.random.uniform(second, (D,), jnp.float32, -0.5, 0.5))
    full = jnp.clip(jax.random.normal(first, (SEQUENCE_TOKENS, D), jnp.float32), -5.0, 5.0) * rising * rough
    return full.astype(jnp.bfloat16)


def draw_values(key, part):
    first, second = jax.random.split(jax.random.fold_in(key, 41), 2)
    head_place = (jnp.arange(VALS) // DV).astype(jnp.float32)
    rising = 3.0 ** (head_place / (HEADS - 1))
    rough = jnp.exp(jax.random.uniform(second, (VALS,), jnp.float32, -0.5, 0.5))
    base = jnp.clip(jax.random.normal(first, (SEQUENCE_TOKENS, VALS), jnp.float32), -5.0, 5.0)
    return (base * rising * rough).astype(jnp.bfloat16)


def draw_input_gate(key, part):
    first = jax.random.fold_in(jax.random.fold_in(key, 23), 0)
    base = jnp.clip(1.5 * jax.random.normal(first, (SEQUENCE_TOKENS, HEADS), jnp.float32), -9.0, 9.0)
    return base


def draw_forget_gate(key, part):
    partition_key = jax.random.split(jax.random.fold_in(key, 37), 6)
    fast_share = 0.5
    fast = jax.random.uniform(partition_key[0], (HEADS,), jnp.float32) < fast_share
    fast_rate = 1.0 / jax.random.uniform(partition_key[1], (HEADS,), jnp.float32, 30.0, 100.0)
    slow_rate = 0.12 * math.log(10.0) / SEQUENCE_TOKENS
    factor = jnp.exp(jax.random.uniform(partition_key[2], (SEQUENCE_TOKENS // TOK_DEV, 1), jnp.float32, -math.log(2.0), math.log(2.0)))
    factor = jnp.repeat(factor, TOK_DEV, axis=0)
    speed_ratio = jnp.where(fast, fast_rate, slow_rate)[None, :] * factor
    position_slots = jax.random.randint(partition_key[3], (3,), 0, SEQUENCE_TOKENS)
    spike_events = jnp.any(jnp.arange(SEQUENCE_TOKENS)[:, None] == position_slots[None, :], axis=1)[:, None]
    spike_frequency = -jnp.log(jax.random.uniform(partition_key[4], (SEQUENCE_TOKENS, 1), jnp.float32, 0.55, 0.8))
    speed_ratio = jnp.where(spike_events, spike_frequency, speed_ratio)
    noise = jnp.clip(0.7 * jax.random.normal(partition_key[5], (SEQUENCE_TOKENS, HEADS), jnp.float32), -2.0, 2.0)
    return -jnp.log(jnp.expm1(speed_ratio)) + noise


def block_levels(key, dims, cuts, least, top_value):
    loudness, own = 1.0, jax.random.fold_in(key, 6)
    for axis_at, blocks in cuts:
        heights = jnp.exp(jax.random.uniform(jax.random.fold_in(own, axis_at), (blocks,), jnp.float32, least / len(cuts), top_value / len(cuts)))
        loudness = loudness * jnp.repeat(heights, dims[axis_at] // blocks).reshape([-1 if axis == axis_at else 1 for axis in range(len(dims))])
    return loudness


def normal_values(rng, dims, scale, reach, shards=(), kind=jnp.bfloat16):
    drawn = scale * jax.random.normal(rng, dims, jnp.float32)
    if shards:
        drawn = drawn * block_levels(rng, dims, shards, -0.22, 0.18)
    return jnp.clip(drawn, -reach, reach).astype(kind)


def setup_inputs(seed: int = 0) -> dict:
    seeds = jax.random.split(jax.random.key(seed), 14)
    return {
        "stream": draw_stream(jax.random.fold_in(seeds[13], 71), 0),
        "queries": normal_values(seeds[1], (SEQUENCE_TOKENS, HEADS * DQK), 1.0, 6.0, ((0, 8), (1, 4))),
        "keys": normal_values(seeds[2], (SEQUENCE_TOKENS, HEADS * DQK), 1.0, 6.0, ((0, 8), (1, 4))),
        "values": draw_values(jax.random.fold_in(seeds[13], 71), 0),
        "out_gate": normal_values(seeds[4], (SEQUENCE_TOKENS, VALS), 1.5, 8.0, ((0, 8), (1, 4))),
        "input_gate": draw_input_gate(jax.random.fold_in(seeds[13], 71), 0),
        "forget_gate": draw_forget_gate(jax.random.fold_in(seeds[13], 71), 0),
        "head_gain": jnp.clip(1.0 + 0.18 * jax.random.normal(seeds[7], (VALS,), jnp.float32), 0.1, 1.9),
        "w_out": normal_values(seeds[8], (VALS, D), VALS ** -0.5, 0.125, ((0, 4),)),
        "ffn_gain": jnp.clip(1.0 + 0.18 * jax.random.normal(seeds[9], (D,), jnp.float32), 0.1, 1.9),
        "w_gate": normal_values(seeds[10], (D, FF), D ** -0.5, 0.125, ((0, 8), (1, 4))),
        "w_up": normal_values(seeds[11], (D, FF), D ** -0.5, 0.125, ((0, 8), (1, 4))),
        "w_down": normal_values(seeds[12], (FF, D), FF ** -0.5, 0.078125, ((0, 4), (1, 8))),
    }


precise = lax.Precision.HIGHEST
norm_eps = 1e-06
very_low = -1e+30

def block_summary(key_blk, value_blk, input_blk, decay_sum):
    decay_total = decay_sum[..., -1]
    log_weight = decay_total[..., None] - decay_sum + input_blk
    weight_peak = lax.optimization_barrier(jnp.max(log_weight, axis=-1))
    weights = jnp.exp(log_weight - weight_peak[..., None])
    state_mat = jnp.einsum('...ld,...le->...de', weights[..., None] * key_blk, value_blk, precision=precise)
    state_vec = jnp.einsum('...l,...ld->...d', weights, key_blk, precision=precise)
    return (state_mat, state_vec, weight_peak, decay_total)

def combine(earlier, later):
    ceiling = jnp.maximum(later[3] + earlier[2], later[2])
    former = jnp.exp(later[3] + earlier[2] - ceiling)
    latter = jnp.exp(later[2] - ceiling)
    return (former[..., None, None] * earlier[0] + latter[..., None, None] * later[0], former[..., None] * earlier[1] + latter[..., None] * later[1], ceiling, earlier[3] + later[3])

def block_output(query_blk, key_blk, value_blk, input_blk, decay_sum, state_mat, state_vec, state_peak):
    block_len = query_blk.shape[-2]
    causal = jnp.tril(jnp.ones((block_len, block_len), jnp.bool_))
    log_pair = jnp.where(causal, decay_sum[..., :, None] - decay_sum[..., None, :] + input_blk[..., None, :], -jnp.inf)
    log_carry = decay_sum + state_peak[..., None]
    row_peak = jnp.maximum(log_carry, lax.optimization_barrier(jnp.max(log_pair, axis=-1)))
    scores = jnp.einsum('...ld,...sd->...ls', query_blk, key_blk, precision=precise) * jnp.exp(log_pair - row_peak[..., None])
    carried = jnp.exp(log_carry - row_peak)
    numer = jnp.einsum('...ls,...se->...le', scores, value_blk, precision=precise) + carried[..., None] * jnp.einsum('...ld,...de->...le', query_blk, state_mat, precision=precise)
    normer = lax.optimization_barrier(jnp.sum(scores, axis=-1)) + carried * jnp.einsum('...ld,...d->...l', query_blk, state_vec, precision=precise)
    denom = jnp.maximum(jnp.abs(normer), jnp.exp(-row_peak))
    return numer / denom[..., None]

def reference(stream, queries, keys, values, out_gate, input_gate, forget_gate, head_gain, w_out, ffn_gain, w_gate, w_up, w_down):
    blocks = SEQUENCE_TOKENS // BLOCK

    def to_blocks(array, col_width):
        return array.reshape(blocks, BLOCK, HEADS, col_width).transpose(0, 2, 1, 3)
    query_all = to_blocks(queries, DQK)
    key_all = to_blocks(keys, DQK)
    value_all = to_blocks(values, DV)
    input_all = input_gate.reshape(blocks, BLOCK, HEADS).transpose(0, 2, 1)
    forget_all = forget_gate.reshape(blocks, BLOCK, HEADS).transpose(0, 2, 1)

    def advance(carry, pieces):
        query_blk = pieces[0].astype(jnp.float32) * DQK ** (-0.5)
        key_blk = pieces[1].astype(jnp.float32)
        value_blk = pieces[2].astype(jnp.float32)
        decay_sum = jnp.cumsum(jax.nn.log_sigmoid(pieces[4]), axis=-1)
        output = block_output(query_blk, key_blk, value_blk, pieces[3], decay_sum, carry[0], carry[1], carry[2])
        return (combine(carry, block_summary(key_blk, value_blk, pieces[3], decay_sum)), output)
    start = (jnp.zeros((HEADS, DQK, DV), jnp.float32), jnp.zeros((HEADS, DQK), jnp.float32), jnp.full((HEADS,), very_low, jnp.float32), jnp.zeros((HEADS,), jnp.float32))
    _, mixed_heads = lax.scan(advance, start, (query_all, key_all, value_all, input_all, forget_all))
    head_rows = mixed_heads.transpose(0, 2, 1, 3).reshape(SEQUENCE_TOKENS, HEADS, DV)
    mean_sq = lax.optimization_barrier(jnp.mean(head_rows * head_rows, axis=(1, 2), keepdims=True))
    gated = head_rows * lax.rsqrt(mean_sq + norm_eps) * head_gain.reshape(HEADS, DV) * jax.nn.sigmoid(out_gate.astype(jnp.float32).reshape(SEQUENCE_TOKENS, HEADS, DV))
    heads_out = gated.reshape(SEQUENCE_TOKENS, HEADS * DV).astype(jnp.bfloat16)
    group = HEADS * DV // N_TP
    mixer = jnp.zeros((SEQUENCE_TOKENS, D), jnp.float32)
    for member in range(N_TP):
        partial_value = jnp.dot(heads_out[:, member * group:(member + 1) * group], w_out[member * group:(member + 1) * group], preferred_element_type=jnp.float32).astype(jnp.bfloat16)
        mixer = mixer + lax.optimization_barrier(partial_value).astype(jnp.float32)
    resid = (stream.astype(jnp.float32) + mixer).astype(jnp.bfloat16)
    hidden_group = FF // N_TP

    def channel_mix(rows_in):
        rows_float = rows_in.astype(jnp.float32)
        normed = (rows_float * lax.rsqrt(lax.optimization_barrier(jnp.mean(rows_float * rows_float, axis=-1, keepdims=True)) + norm_eps) * ffn_gain).astype(jnp.bfloat16)
        gate_act = jnp.dot(normed, w_gate, preferred_element_type=jnp.float32)
        up_act = jnp.dot(normed, w_up, preferred_element_type=jnp.float32)
        hidden = (jax.nn.silu(gate_act) * up_act).astype(jnp.bfloat16)
        totals = jnp.zeros((rows_in.shape[0], D), jnp.float32)
        for member in range(N_TP):
            partial_value = jnp.dot(hidden[:, member * hidden_group:(member + 1) * hidden_group], w_down[member * hidden_group:(member + 1) * hidden_group], preferred_element_type=jnp.float32).astype(jnp.bfloat16)
            totals = totals + lax.optimization_barrier(partial_value).astype(jnp.float32)
        return (rows_float + totals).astype(jnp.bfloat16)
    mixed = lax.map(channel_mix, resid.reshape(N_SP, TOK_DEV, D))
    return mixed.reshape(SEQUENCE_TOKENS, D)
```

```python
import jax
import jax.numpy as jnp
from jax import lax
from jax.experimental import pallas as pl
from jax.experimental.pallas import tpu as pltpu
from jax.sharding import PartitionSpec as P

DQK = 128
DV = 256
EXTRA = 16
norm_eps = 1e-06
very_low = -1e30
f32 = jnp.float32
bf16 = jnp.bfloat16
AXES = ("sp", "tp")


def dot(a, b, ca=1, cb=0):
    return lax.dot_general(a, b, (((ca,), (cb,)), ((), ())), preferred_element_type=f32)


def two_terms(x):
    hi = x.astype(bf16)
    return hi, (x - hi.astype(f32)).astype(bf16)


def three_terms(x):
    hi = x.astype(bf16).astype(f32)
    mid = (x - hi).astype(bf16).astype(f32)
    return hi, mid, x - hi - mid


def iota(shape, dim):
    return lax.broadcasted_iota(jnp.int32, shape, dim)


def as_row(col, width):
    eye = iota((col.shape[0], width), 0) == iota((col.shape[0], width), 1)
    return jnp.sum(jnp.where(eye, col, 0.0), axis=0, keepdims=True)


def as_col(row, height):
    eye = iota((height, row.shape[1]), 0) == iota((height, row.shape[1]), 1)
    return jnp.sum(jnp.where(eye, row, 0.0), axis=1, keepdims=True)


def log_sigmoid(x):
    return jnp.minimum(x, 0.0) - jnp.log1p(jnp.exp(-jnp.abs(x)))


def decays(forget_col):
    rows = forget_col.shape[0]
    causal = iota((rows, rows), 1) <= iota((rows, rows), 0)
    log_forget = log_sigmoid(forget_col)
    decay_col = jnp.sum(jnp.where(causal, as_row(log_forget, rows), 0.0), axis=1, keepdims=True)
    decay_row = as_row(decay_col, rows)
    return causal, decay_col, decay_row


def pack_extra(vec, peak, total):
    width = 2 * vec.shape[1]
    row = iota((EXTRA, width), 0)
    left = iota((EXTRA, width), 1) < vec.shape[1]
    out = jnp.zeros((EXTRA, width), f32)
    hi, mid, lo = (jnp.concatenate([part, part], axis=1) for part in three_terms(vec))
    out = jnp.where(row == 0, jnp.where(left, hi, mid), out)
    out = jnp.where(row == 1, lo, out)
    for place, part in enumerate(three_terms(peak) + three_terms(total)):
        out = jnp.where(row == 2 + place, part, out)
    return out.astype(bf16)


def unpack_extra(block):
    block = block.astype(f32)
    vec = block[0:1, :DQK] + block[0:1, DQK : 2 * DQK] + block[1:2, :DQK]
    peak = block[2:3, :1] + block[3:4, :1] + block[4:5, :1]
    total = block[5:6, :1] + block[6:7, :1] + block[7:8, :1]
    return vec, peak, total


def summary_kernel(k_ref, v_ref, i_ref, f_ref, out_ref):
    rows = k_ref.shape[0]
    for h in range(i_ref.shape[1]):
        _, decay_col, _ = decays(f_ref[:, h : h + 1])
        total = decay_col[rows - 1 : rows, :]
        log_weight = total - decay_col + i_ref[:, h : h + 1]
        peak = jnp.max(log_weight, axis=0, keepdims=True)
        weighted = k_ref[:, h * DQK : (h + 1) * DQK].astype(f32) * jnp.exp(log_weight - peak)
        hi, lo = two_terms(weighted)
        value = v_ref[:, h * DV : (h + 1) * DV]
        state = dot(hi, value, 0, 0) + dot(lo, value, 0, 0)
        out_ref[h, :DQK, :] = state.astype(bf16)
        out_ref[h, DQK:, :] = pack_extra(jnp.sum(weighted, axis=0, keepdims=True), peak, total)


def join_kernel(own_ref, other_ref, out_ref):
    first = lax.rem(lax.axis_index("sp"), 2) == 0
    for h in range(own_ref.shape[0]):
        own_n, own_m, own_d = unpack_extra(own_ref[h, DQK:, :])
        oth_n, oth_m, oth_d = unpack_extra(other_ref[h, DQK:, :])
        own_log = own_m + jnp.where(first, oth_d, 0.0)
        oth_log = oth_m + jnp.where(first, 0.0, own_d)
        peak = jnp.maximum(own_log, oth_log)
        own_w, oth_w = jnp.exp(own_log - peak), jnp.exp(oth_log - peak)
        state = own_w * own_ref[h, :DQK, :].astype(f32) + oth_w * other_ref[h, :DQK, :].astype(f32)
        out_ref[h, :DQK, :] = state.astype(bf16)
        out_ref[h, DQK:, :] = pack_extra(own_w * own_n + oth_w * oth_n, peak, own_d + oth_d)


def intra_kernel(q_ref, k_ref, v_ref, i_ref, f_ref, num_ref, aux_ref):
    rows = q_ref.shape[0]
    lane = iota((rows, 128), 1)
    aux = jnp.zeros((rows, 128), f32)
    for h in range(i_ref.shape[1]):
        causal, decay_col, decay_row = decays(f_ref[:, h : h + 1])
        in_row = as_row(i_ref[:, h : h + 1], rows)
        log_pair = jnp.where(causal, decay_col - decay_row + in_row, -jnp.inf)
        peak = jnp.max(log_pair, axis=1, keepdims=True)
        scores = dot(q_ref[:, h * DQK : (h + 1) * DQK], k_ref[:, h * DQK : (h + 1) * DQK], 1, 1)
        scores = scores * (DQK**-0.5) * jnp.exp(log_pair - peak)
        hi, lo = two_terms(scores)
        value = v_ref[:, h * DV : (h + 1) * DV]
        num_ref[:, h * DV : (h + 1) * DV] = dot(hi, value) + dot(lo, value)
        for place, part in enumerate((decay_col, peak, jnp.sum(scores, axis=1, keepdims=True))):
            aux = jnp.where(lane == 3 * h + place, part, aux)
    aux_ref[...] = aux


def output_kernel(*refs):
    q_ref, num_ref, aux_ref, og_ref, gain_ref, w_ref, mate_ref = refs[:7]
    tp = lax.axis_size("tp")
    sent = lax.axis_size("sp") // 2 - 1
    earlier, outs, scratch = refs[7 : 7 + sent], refs[7 + sent : -1], refs[-1]
    s, t = lax.axis_index("sp"), lax.axis_index("tp")
    zi, second = s // 2, lax.rem(s, 2) == 1
    rows = q_ref.shape[0]
    heads = mate_ref.shape[0]
    square = jnp.zeros((rows, 1), f32)
    gated = []
    for h in range(heads):
        mate_n, mate_m, mate_d = unpack_extra(mate_ref[h, DQK:, :])
        later = jnp.where(second, mate_d, 0.0)
        logs = [jnp.where(second, mate_m, very_low)]
        keep = [second]
        vecs = [mate_n]
        for k, ref in enumerate(earlier):
            vec, peak, total = unpack_extra(ref[h, DQK:, :])
            valid = zi >= k + 1
            logs.append(jnp.where(valid, peak + later, very_low))
            later = later + total
            keep.append(valid)
            vecs.append(vec)
        top = logs[0]
        for part in logs[1:]:
            top = jnp.maximum(top, part)
        weights = [jnp.where(ok, jnp.exp(part - top), 0.0) for ok, part in zip(keep, logs)]
        state = weights[0] * mate_ref[h, :DQK, :].astype(f32)
        vec = weights[0] * vecs[0]
        for weight, ref, part in zip(weights[1:], earlier, vecs[1:]):
            state = state + weight * ref[h, :DQK, :].astype(f32)
            vec = vec + weight * part
        query = q_ref[:, h * DQK : (h + 1) * DQK]
        hi, lo = two_terms(state)
        carried = (dot(query, hi) + dot(query, lo)) * (DQK**-0.5)
        carried_n = jnp.sum(query.astype(f32) * vec, axis=1, keepdims=True) * (DQK**-0.5)
        decay_col, peak, normer = (aux_ref[:, 3 * h + i : 3 * h + i + 1] for i in range(3))
        log_carry = decay_col + top
        row_peak = jnp.maximum(log_carry, peak)
        a, b = jnp.exp(peak - row_peak), jnp.exp(log_carry - row_peak)
        normer = a * normer + b * carried_n
        denom = jnp.maximum(jnp.abs(normer), jnp.exp(-row_peak))
        cell = (a * num_ref[:, h * DV : (h + 1) * DV] + b * carried) / denom
        square = square + jnp.sum(cell * cell, axis=1, keepdims=True)
        gate = jax.nn.sigmoid(og_ref[:, h * DV : (h + 1) * DV].astype(f32))
        gated.append((cell * gain_ref[:, h * DV : (h + 1) * DV] * gate).astype(bf16))
    width = w_ref.shape[1] // tp
    hi, mid, lo = three_terms(as_row(square, width))
    row = iota((EXTRA, width), 0)
    extra = jnp.where(row == 0, hi, jnp.where(row == 1, mid, jnp.where(row == 2, lo, 0.0)))
    for j in range(tp):
        part = sum(
            dot(gated[h], w_ref[h * DV : (h + 1) * DV, j * width : (j + 1) * width])
            for h in range(heads)
        )
        scratch[j, :, :] = part.astype(bf16)
    for j in range(tp):
        outs[j][:rows, :] = scratch[jnp.bitwise_xor(t, j)]
        outs[j][rows:, :] = extra.astype(bf16)


def resid_kernel(*refs):
    stream_ref, parts, out_ref = refs[0], refs[1:-1], refs[-1]
    rows, width = stream_ref.shape
    total = parts[0][...].astype(f32)
    for ref in parts[1:]:
        total = total + ref[...].astype(f32)
    ends = total[rows:, :]
    square = as_col(ends[0:1, :] + ends[1:2, :] + ends[2:3, :], rows)
    channels = width * lax.axis_size("tp")
    scale = lax.rsqrt(square / channels + norm_eps)
    out_ref[...] = (stream_ref[...].astype(f32) + total[:rows, :] * scale).astype(bf16)


def prepare_kernel(g_ref, u_ref, d_ref, *refs):
    groups = lax.axis_size("sp") // 2
    zi = lax.axis_index("sp") // 2
    pairs, downs, g_all, u_all, d_all = refs[:groups], refs[groups : 2 * groups], *refs[2 * groups :]
    size = d_ref.shape[0] // groups
    g_turned, u_turned = g_ref[...].T, u_ref[...].T
    for place in range(groups):
        g_all[place] = g_turned[place * size : (place + 1) * size, :]
        u_all[place] = u_turned[place * size : (place + 1) * size, :]
        d_all[place] = d_ref[place * size : (place + 1) * size, :]
    for k in range(groups):
        place = lax.rem(zi + k, groups)
        pairs[k][0] = g_all[place]
        pairs[k][1] = u_all[place]
        downs[k][...] = d_all[place]


def mlp_kernel(*refs):
    tp, sp = lax.axis_size("tp"), lax.axis_size("sp")
    groups = sp // 2
    s, t = lax.axis_index("sp"), lax.axis_index("tp")
    zi, y = s // 2, lax.rem(s, 2)
    gain_ref, rows_in = refs[0], refs[1 : 1 + tp]
    pairs, downs = refs[1 + tp : 1 + tp + sp], refs[1 + tp + sp : 1 + tp + 2 * sp]
    near_ref, far_ref, normed, outs = refs[1 + tp + 2 * sp :]
    rows, width = rows_in[0].shape
    deep = normed.shape[2]
    per = width // deep
    square = jnp.zeros((rows, 1), f32)
    for ref in rows_in:
        part = ref[...].astype(f32)
        square = square + jnp.sum(part * part, axis=1, keepdims=True)
    scale = lax.rsqrt(square / (width * tp) + norm_eps)
    for j in range(tp):
        base = jnp.bitwise_xor(t, j) * per
        for i in range(per):
            part = rows_in[j][:, i * deep : (i + 1) * deep].astype(f32)
            normed[base + i] = (part * scale * gain_ref[base + i]).astype(bf16)
    gate = up = None
    for k in range(groups):
        for side in range(2):
            place = lax.rem(zi - k + groups, groups) * 2 + jnp.bitwise_xor(y, side)
            part = normed[place]
            piece = pairs[2 * k + side]
            g, u = dot(part, piece[0], 1, 1), dot(part, piece[1], 1, 1)
            gate, up = (g, u) if gate is None else (gate + g, up + u)
    hidden = (gate / (1.0 + jnp.exp(-gate)) * up).astype(bf16)
    for k in range(groups):
        for side in range(2):
            place = lax.rem(zi - k + groups, groups) * 2 + jnp.bitwise_xor(y, side)
            outs[place] = dot(hidden, downs[2 * k + side][...]).astype(bf16)
    for j in range(tp):
        base = jnp.bitwise_xor(t, j) * per
        target = far_ref if j & 1 else near_ref
        for i in range(per):
            target[j // 2, :, i * deep : (i + 1) * deep] = outs[base + i]


VMEM = pltpu.VMEM


def call(kernel, out_shape, *args, scratch=(), name=None):
    return pl.pallas_call(
        kernel,
        out_shape=out_shape,
        in_specs=[pl.BlockSpec(memory_space=VMEM)] * len(args),
        out_specs=jax.tree.map(lambda _: pl.BlockSpec(memory_space=VMEM), out_shape),
        scratch_shapes=list(scratch),
        compiler_params=pltpu.CompilerParams(vmem_limit_bytes=40 * 2**20),
        name=name,
    )(*args)


def local(
    stream, queries, keys, values, out_gate, input_gate, forget_gate,
    head_gain, w_out, ffn_gain, w_gate, w_up, w_down,
):
    sp, tp = lax.axis_size("sp"), lax.axis_size("tp")
    groups = sp // 2
    rows, width = stream.shape
    heads = input_gate.shape[1]
    deep = w_gate.shape[0]
    size = w_down.shape[0] // groups

    def shape(*dims, dtype=bf16):
        return jax.ShapeDtypeStruct(dims, dtype)

    def move(x, send):
        pairs = []
        for s in range(sp):
            for t in range(tp):
                to = send(s // 2, s % 2, t)
                if to is not None:
                    pairs.append((s * tp + t, (to[0] * 2 + to[1]) * tp + to[2]))
        return lax.ppermute(x, AXES, pairs)

    def mate(x):
        return move(x, lambda z, y, t: (z, 1 - y, t))

    def turn(x, k):
        return move(x, lambda z, y, t: ((z + k) % groups, y, t))

    def ahead(x, k):
        return move(x, lambda z, y, t: (z + k, y, t) if z + k < groups else None)

    def flip(x, j):
        return move(x, lambda z, y, t: (z, y, t ^ j))

    packed = shape(heads, DQK + EXTRA, DV)
    own = call(summary_kernel, packed, keys, values, input_gate, forget_gate, name="summary")
    other = mate(own)
    prepared = call(
        prepare_kernel,
        [shape(2, size, deep)] * groups + [shape(size, deep)] * groups,
        w_gate, w_up, w_down,
        scratch=[VMEM((groups, size, deep), bf16)] * 3,
        name="prepare",
    )
    pairs, downs = prepared[:groups], prepared[groups:]
    numer, aux = call(
        intra_kernel,
        [shape(rows, heads * DV, dtype=f32), shape(rows, 128, dtype=f32)],
        queries, keys, values, input_gate, forget_gate,
        name="intra",
    )
    joined = call(join_kernel, packed, own, other, name="join")
    earlier = [ahead(joined, k) for k in range(1, groups)]
    pairs_in, downs_in = [], []
    for k in range(groups):
        pair = turn(pairs[k], k) if k else pairs[0]
        pairs_in += [pair, mate(pair)]
    for k in range(groups):
        down = turn(downs[k], k) if k else downs[0]
        downs_in += [down, mate(down)]
    parts = call(
        output_kernel,
        [shape(rows + EXTRA, width)] * tp,
        queries, numer, aux, out_gate, head_gain.reshape(1, -1), w_out, other, *earlier,
        scratch=[VMEM((tp, rows, width), bf16)],
        name="output",
    )
    parts = [parts[0]] + [flip(parts[j], j) for j in range(1, tp)]
    resid = call(resid_kernel, shape(rows, width), stream, *parts, name="resid")
    gain = ffn_gain.reshape(sp, 1, deep)
    total = resid.astype(f32)
    blocks = [resid] + [turn(resid, k) for k in range(1, groups)]
    for k in range(groups):
        have = {0: blocks[k]}
        bit = tp // 2
        while bit:
            have.update({j ^ bit: flip(part, bit) for j, part in list(have.items())})
            bit //= 2
        near, far = call(
            mlp_kernel,
            [shape(tp // 2, rows, width)] * 2,
            gain, *[have[j] for j in range(tp)], *pairs_in, *downs_in,
            scratch=[VMEM((sp, rows, deep), bf16)] * 2,
            name="mlp",
        )
        got = flip(far, 1)
        summed = near.astype(f32) + got.astype(f32)
        bit = tp // 2
        while bit > 1:
            half = bit // 2
            got = flip(summed[half:].astype(bf16), bit)
            summed = summed[:half] + got.astype(f32)
            bit = half
        block = summed[0]
        if k:
            block = turn(block.astype(bf16), groups - k).astype(f32)
        total = total + block
    return total.astype(bf16)


def solution(mesh):
    both = P("sp", "tp")
    in_specs = (
        both, both, both, both, both, both, both,
        P("tp"), P("tp", None), P(), both, both, P("tp", "sp"),
    )
    return jax.shard_map(local, mesh=mesh, in_specs=in_specs, out_specs=both, check_vma=False)
```
